32 devices in a mesh: rep: 4 (over z), fs: 4 (over y, x), tp: 2 (over core).
Axes of the slice: x: 2, y: 2, z: 4, core: 2. Of those that a mesh axis runs over, the one named last changes fastest.
Arguments:
- hidden_in: bfloat16 [2048, 2048], P('rep'), may hold values from -6 to 6
- cotangent: bfloat16 [2048, 2048], P('rep'), may hold values from -3 to 3
- w_up: bfloat16 [2048, 8192], P('rep', ('fs', 'tp')), may hold values from -0.125 to 0.125
- w_down: bfloat16 [8192, 2048], P(('fs', 'tp'), 'rep'), may hold values from -0.0625 to 0.0625
Outputs:
- input_grad: bfloat16 [2048, 2048], P('rep')
- up_grad: float32 [2048, 8192], P('rep', ('fs', 'tp'))
- down_grad: float32 [8192, 2048], P(('fs', 'tp'), 'rep')
The draws below stay inside these ranges and needn't reach their ends.
All inputs are finite; a program needn't handle non-finite values.
Results may differ from the reference program's by a relative error of at most 0.017.
Values may be sent and summed in bfloat16 or wider, within the bound.
A program may use at most 64 MiB of HBM per device.

```python
import jax
import jax.numpy as jnp
from jax import lax

D = 2048
FF = 8192
TOKENS = 2048
N_FS = 4
N_TP = 2


def strengthened(drawn, key, source, target, parts, factor):
    def block_of(dim):
        return (jnp.arange(drawn.shape[dim]) // (drawn.shape[dim] // parts)).reshape((-1,) + (1,) * (drawn.ndim - 1 - dim))

    near = jax.random.permutation(key, parts)[block_of(target)]
    other_side = (block_of(target) + parts // 2) % parts
    return jnp.where((block_of(source) == near) | (block_of(source) == other_side), factor * drawn, drawn)


def level_of(stream_key, dims, pieces, low, largest):
    level = 1.0
    for position, parts in pieces:
        steps = jax.random.uniform(jax.random.fold_in(jax.random.fold_in(stream_key, 6), position), (parts,), jnp.float32, low / len(pieces), largest / len(pieces))
        level = level * jnp.repeat(jnp.exp(steps), dims[position] // parts).reshape((-1,) + (1,) * (len(dims) - 1 - position))
    return level


def noise(key, extent, width, reach, pieces=(), dtype=jnp.bfloat16):
    drawn = width * jax.random.normal(key, extent, jnp.float32)
    if pieces:
        drawn = drawn * level_of(key, extent, pieces, -0.22, 0.18)
    return jnp.clip(drawn, -reach, reach).astype(dtype)


def heavy_noise(key, shape, width, bound, split, heavy, kind=jnp.bfloat16):
    values = width * jax.random.normal(key, shape, jnp.float32)
    if split:
        values = values * level_of(key, shape, split, -0.22, 0.18)
    return jnp.clip(strengthened(values, jax.random.fold_in(key, 3), *heavy), -bound, bound).astype(kind)


def setup_inputs(seed: int = 0) -> dict:
    splits = jax.random.split(jax.random.key(seed), 5)
    hidden_in = heavy_noise(splits[0], (TOKENS, D), 1.0, 6.0, ((0, 4),), (0, 1, 4, 2.0))
    cotangent = heavy_noise(splits[1], (TOKENS, D), 0.5, 3.0, ((0, 4),), (0, 1, 4, 2.0))
    w_up = noise(splits[2], (D, FF), D ** -0.5, 0.125, ((0, 4), (1, 8)))
    w_down = noise(splits[3], (FF, D), FF ** -0.5, 0.0625, ((0, 8), (1, 4)))
    return dict(hidden_in=hidden_in, cotangent=cotangent, w_up=w_up, w_down=w_down)


def contract_last(left, right):
    return lax.dot_general(left, right, (((1,), (1,)), ((), ())), preferred_element_type=jnp.float32)


def contract_first(left, right):
    return lax.dot_general(left, right, (((0,), (0,)), ((), ())), preferred_element_type=jnp.float32)


def reference(hidden_in, cotangent, w_up, w_down):
    blocks = N_FS * N_TP
    block_cols = FF // blocks
    up_blocks = jnp.transpose(w_up.reshape(D, blocks, block_cols), (1, 0, 2))
    down_blocks = w_down.reshape(blocks, block_cols, D)

    def one_block(summed, weights):
        up_part, down_part = weights
        preact = jnp.dot(hidden_in, up_part, preferred_element_type=jnp.float32)
        back_grad = contract_last(cotangent, down_part)
        active = jnp.maximum(preact, 0.0)
        hidden = (active * active).astype(jnp.bfloat16)
        slopes = (2.0 * active * back_grad).astype(jnp.bfloat16)
        part_sum = lax.optimization_barrier(contract_last(slopes, up_part).astype(jnp.bfloat16))
        summed = summed + part_sum.astype(jnp.float32)
        grad_upper = contract_first(hidden_in, slopes)
        grad_lower = contract_first(hidden, cotangent)
        return summed, (grad_upper, grad_lower)

    summed, (grads_upper, grads_lower) = lax.scan(
        one_block, jnp.zeros((TOKENS, D), jnp.float32), (up_blocks, down_blocks))
    input_grad = summed.astype(jnp.bfloat16)
    up_grad = jnp.transpose(grads_upper, (1, 0, 2)).reshape(D, FF)
    down_grad = grads_lower.reshape(FF, D)
    return (input_grad, up_grad, down_grad)
```

```python
import functools

import jax
import jax.numpy as jnp
from jax import lax
from jax.experimental import pallas as pl
from jax.experimental.pallas import tpu as pltpu
from jax.sharding import PartitionSpec as P

MESH = pl.DeviceIdType.MESH
BF16, F32 = jnp.bfloat16, jnp.float32


def contract_last(left, right):
    return lax.dot_general(left, right, (((1,), (1,)), ((), ())), preferred_element_type=F32)


def contract_first(left, right):
    return lax.dot_general(left, right, (((0,), (0,)), ((), ())), preferred_element_type=F32)


def plain(hidden_in, cotangent, w_up, w_down):
    up_full = lax.all_gather(w_up, "rep", axis=0, tiled=True)
    back_grad = contract_last(cotangent, lax.all_gather(w_down, "rep", axis=1, tiled=True))
    preact = jnp.dot(hidden_in, up_full, preferred_element_type=F32)
    active = jnp.maximum(preact, 0.0)
    hidden = (active * active).astype(BF16)
    slopes = (2.0 * active * back_grad).astype(BF16)
    grad_upper = lax.psum_scatter(
        contract_first(hidden_in, slopes).astype(BF16), "rep", scatter_dimension=0, tiled=True
    ).astype(F32)
    lower_rows = lax.psum_scatter(
        contract_first(cotangent, hidden).astype(BF16), "rep", scatter_dimension=0, tiled=True
    ).astype(F32)
    partial_sum = contract_last(slopes, up_full).astype(BF16)
    input_grad = lax.psum(partial_sum, ("fs", "tp")).astype(F32).astype(BF16)
    return (input_grad, grad_upper, lower_rows.T)


SEMS = 256


def kernel(
    R, x_ref, g_ref, wu_in, wd_in,
    ig_ref, ru_ref, rd_ref,
    tx, tg, wu, wd, act, slopes, s_t, h_t, part, r0, r1, r2, r3, ug, dg,
    send_sems, recv_sems, local_sems,
):
    z, f, c = lax.axis_index("rep"), lax.axis_index("fs"), lax.axis_index("tp")
    tl, D = x_ref.shape
    dl, fl = wu_in.shape
    h = fl // R
    pr = tl // 8
    xx, yy = lax.rem(f, 2), lax.div(f, 2)
    fx, fy = yy * 2 + (1 - xx), (1 - yy) * 2 + xx
    f1 = fx * (1 - c) + fy * c
    f2 = fy * (1 - c) + fx * c
    f3 = 3 - f
    order = [d for d in (1, 3, 2) if d < R] if R == 4 else list(range(1, R))

    pending = []
    keys = {}

    def key_of(key):
        return keys.setdefault(key, len(keys))

    def dev(zz=None, ff=None, cc=None):
        return {"rep": z if zz is None else zz, "fs": f if ff is None else ff, "tp": c if cc is None else cc}

    def send(src, dst, device, key):
        copy = pltpu.make_async_remote_copy(
            src_ref=src, dst_ref=dst, send_sem=send_sems.at[len(pending)],
            recv_sem=recv_sems.at[key_of(key)], device_id=device, device_id_type=MESH)
        copy.start()
        pending.append(copy)

    def arrived(dst, key):
        pltpu.make_async_remote_copy(
            src_ref=dst, dst_ref=dst, send_sem=send_sems.at[0],
            recv_sem=recv_sems.at[key_of(key)], device_id=dev(cc=1 - c), device_id_type=MESH).wait_recv()

    def plane(d):
        return lax.rem(z + d, R)

    def rows(zz, ff, cc):
        return pl.ds(pl.multiple_of(zz * tl + (cc * 4 + ff) * pr, pr), pr)

    barrier = pltpu.get_barrier_semaphore()
    near = [dev(zz=plane(d)) for d in range(1, R)] + [dev(ff=fx), dev(ff=fy), dev(cc=1 - c)]
    for device in near:
        pl.semaphore_signal(barrier, inc=1, device_id=device, device_id_type=MESH)
    pl.semaphore_wait(barrier, len(near))

    tokens = (tx, tg)
    sources = (x_ref, g_ref)

    def send_tokens(a):
        for d in order:
            send(sources[a].at[pl.ds(pl.multiple_of((c * 4 + f) * pr, pr), pr), :],
                 tokens[a].at[rows(z, f, c), :], dev(zz=plane(d)), ("tok", a, R - d, 0))

    def up_cols(zz):
        return pl.ds(pl.multiple_of(zz * h, h), h)

    def d_block(zz):
        return pl.ds(pl.multiple_of(zz * dl, dl), dl)

    send_tokens(0)
    send_tokens(1)
    for d in order:
        send(wu_in.at[:, up_cols(plane(d))], wu.at[d_block(z), :], dev(zz=plane(d)), ("wu", R - d))
    for d in order:
        send(wd_in.at[up_cols(plane(d)), :], wd.at[:, d_block(z)], dev(zz=plane(d)), ("wd", R - d))

    own_rows = pl.ds(pl.multiple_of(z * tl, tl), tl)
    local = [
        pltpu.make_async_copy(x_ref, tx.at[own_rows, :], local_sems.at[0]),
        pltpu.make_async_copy(g_ref, tg.at[own_rows, :], local_sems.at[1]),
        pltpu.make_async_copy(wu_in.at[:, up_cols(z)], wu.at[d_block(z), :], local_sems.at[2]),
        pltpu.make_async_copy(wd_in.at[up_cols(z), :], wd.at[:, d_block(z)], local_sems.at[3]),
    ]
    for copy in local:
        copy.start()

    def spread(buf, tag, zz):
        def piece(ff, cc):
            return buf.at[rows(zz, ff, cc) if zz is not None else
                          pl.ds(pl.multiple_of((cc * 4 + ff) * pr, pr), pr), :]

        def first():
            mine = piece(f, c)
            send(mine, mine, dev(ff=f1), tag + (1,))
            send(mine, mine, dev(ff=f2), tag + (2,))
            send(mine, mine, dev(cc=1 - c), tag + (4,))

        def second():
            p1, p2 = piece(f1, c), piece(f2, c)
            arrived(p1, tag + (1,))
            send(p1, p1, dev(ff=f2), tag + (3,))
            send(p1, p1, dev(cc=1 - c), tag + (5,))
            arrived(p2, tag + (2,))
            send(p2, p2, dev(cc=1 - c), tag + (6,))

        def third():
            p3 = piece(f3, c)
            arrived(p3, tag + (3,))
            send(p3, p3, dev(cc=1 - c), tag + (7,))

        def last():
            for k, ff in ((4, f), (5, f2), (6, f1), (7, f3)):
                arrived(piece(ff, 1 - c), tag + (k,))

        return first, second, third, last

    lasts = {}
    items = [(a, d) for a in (0, 1) for d in order]
    stages = []
    for a, d in items:
        first, second, third, last = spread(tokens[a], ("tok", a, d), plane(d))

        def opening(a=a, d=d, first=first):
            arrived(tokens[a].at[rows(plane(d), f, c), :], ("tok", a, d, 0))
            first()

        stages.append((opening, second, third))
        lasts[a, d] = last
    for i in range(len(items) + 2):
        for back in (0, 1, 2):
            if 0 <= i - back < len(items):
                stages[i - back][back]()

    for copy in local:
        copy.wait()
    for d in order:
        arrived(wu.at[d_block(plane(d)), :], ("wu", d))
    step = min(tl, 256)

    def up_block(d):
        @pl.loop(0, tl // step)
        def _(i):
            at = pl.ds(pl.multiple_of(plane(d) * tl + i * step, step), step)
            active = jnp.maximum(jnp.dot(tx[at, :], wu[...], preferred_element_type=F32), 0.0)
            act[at, :] = active
            h_t[:, at] = jnp.transpose(active * active).astype(BF16)

    up_block(0)
    for d in order:
        lasts[0, d]()
        up_block(d)
    for d in order:
        lasts[1, d]()

    for d in order + [0]:
        at = d_block(plane(d))
        dg[:, at] = jnp.dot(h_t[...], tg[:, at], preferred_element_type=F32).astype(BF16)
        if d:
            send(dg.at[:, at], rd_ref.at[up_cols(z), :], dev(zz=plane(d)), ("rd", R - d))
        else:
            rd_ref[up_cols(z), :] = dg[:, at]

    for d in order:
        arrived(wd.at[:, d_block(plane(d))], ("wd", d))

    def slope_block(d):
        @pl.loop(0, tl // step)
        def _(i):
            at = pl.ds(pl.multiple_of(plane(d) * tl + i * step, step), step)
            value = 2.0 * act[at, :] * contract_last(tg[at, :], wd[...])
            slopes[at, :] = value.astype(BF16)
            s_t[:, at] = jnp.transpose(value).astype(BF16)

    half = 4 * pr

    def half_rows(d, cc):
        return pl.ds(pl.multiple_of(plane(d) * tl + cc * half, half), half)

    def r0_rows(d):
        return pl.ds(d * half, half)

    for d in order + [0]:
        slope_block(d)

    for d in order + [0]:
        at = d_block(plane(d))
        ug[at, :] = jnp.transpose(jnp.dot(s_t[...], tx[:, at], preferred_element_type=F32)).astype(BF16)
        if d:
            send(ug.at[at, :], ru_ref.at[:, up_cols(z)], dev(zz=plane(d)), ("ru", R - d))
        else:
            ru_ref[:, up_cols(z)] = ug[at, :]

    for d in order + [0]:
        @pl.loop(0, tl // step)
        def _(i):
            at = pl.ds(pl.multiple_of(plane(d) * tl + i * step, step), step)
            part[at, :] = contract_last(slopes[at, :], wu[...]).astype(BF16)
        send(part.at[half_rows(d, 1 - c), :], r0.at[r0_rows(d), :], dev(cc=1 - c), ("r0", d))

    def added(*terms):
        total = terms[0].astype(F32)
        for term in terms[1:]:
            total = total + term.astype(F32)
        return total.astype(BF16)

    def core_sum(d):
        arrived(r0.at[r0_rows(d), :], ("r0", d))
        for ff in (f1, f3, f, f2):
            at = rows(plane(d), ff, c)
            part[at, :] = added(part[at, :], r0[pl.ds(pl.multiple_of(d * half + ff * pr, pr), pr), :])
        for k, ff in ((0, f1), (1, f3)):
            send(part.at[rows(plane(d), ff, c), :], r1.at[d, k], dev(ff=f1), ("r1", d, k))

    def first_sum(d):
        for k, ff in ((1, f2), (0, f)):
            at = rows(plane(d), ff, c)
            arrived(r1.at[d, k], ("r1", d, k))
            part[at, :] = added(part[at, :], r1[d, k])
            if k:
                send(part.at[at, :], r2.at[d], dev(ff=f2), ("r2", d))

    def second_sum(d):
        at = rows(plane(d), f, c)
        arrived(r2.at[d], ("r2", d))
        part[at, :] = added(part[at, :], r2[d])
        if d:
            send(part.at[at, :], r3.at[R - d], dev(zz=plane(d)), ("r3", R - d))

    turns = order + [0]
    chain = (core_sum, first_sum, second_sum)
    for i in range(len(turns) + 2):
        for back in (2, 1, 0):
            if 0 <= i - back < len(turns):
                chain[back](turns[i - back])

    for d in order:
        arrived(r3.at[d], ("r3", d))
    ig_ref[pl.ds(pl.multiple_of((c * 4 + f) * pr, pr), pr), :] = added(
        part[rows(z, f, c), :], *[r3[d] for d in order])
    for stage in spread(ig_ref, ("ig",), None):
        stage()

    for d in order:
        arrived(rd_ref.at[up_cols(plane(d)), :], ("rd", d))
        arrived(ru_ref.at[:, up_cols(plane(d))], ("ru", d))
    for copy in pending:
        copy.wait_send()
    assert len(pending) <= SEMS and len(keys) <= SEMS


def in_planes(R, hidden_in, cotangent, w_up, w_down):
    tl, D = hidden_in.shape
    dl, fl = w_up.shape
    T, h, pr = tl * R, fl // R, tl // 8
    vmem = pl.BlockSpec(memory_space=pltpu.VMEM)
    input_grad, up, down = pl.pallas_call(
        functools.partial(kernel, R),
        out_shape=(
            jax.ShapeDtypeStruct((tl, D), BF16),
            jax.ShapeDtypeStruct((dl, fl), BF16),
            jax.ShapeDtypeStruct((fl, dl), BF16),
        ),
        in_specs=[pl.BlockSpec(memory_space=pl.ANY)] * 4,
        out_specs=(vmem, vmem, vmem),
        scratch_shapes=[
            pltpu.VMEM((T, D), BF16),
            pltpu.VMEM((T, D), BF16),
            pltpu.VMEM((D, h), BF16),
            pltpu.VMEM((h, D), BF16),
            pltpu.VMEM((T, h), F32),
            pltpu.VMEM((T, h), BF16),
            pltpu.VMEM((h, T), BF16),
            pltpu.VMEM((h, T), BF16),
            pltpu.VMEM((T, D), BF16),
            pltpu.VMEM((R * 4 * pr, D), BF16),
            pltpu.VMEM((R, 2, pr, D), BF16),
            pltpu.VMEM((R, pr, D), BF16),
            pltpu.VMEM((R, pr, D), BF16),
            pltpu.VMEM((D, h), BF16),
            pltpu.VMEM((h, D), BF16),
            pltpu.SemaphoreType.DMA((SEMS,)),
            pltpu.SemaphoreType.DMA((SEMS,)),
            pltpu.SemaphoreType.DMA((4,)),
        ],
        compiler_params=pltpu.CompilerParams(
            collective_id=0, has_side_effects=True, vmem_limit_bytes=65000 * 1024
        ),
    )(hidden_in, cotangent, w_up, w_down)
    return input_grad, up.astype(F32), down.astype(F32)


def solution(mesh):
    R, F, C = (mesh.shape[name] for name in ("rep", "fs", "tp"))
    body = functools.partial(in_planes, R) if (F, C) == (4, 2) else plain
    return jax.shard_map(
        body,
        mesh=mesh,
        in_specs=(P("rep", None), P("rep", None), P("rep", ("fs", "tp")), P(("fs", "tp"), "rep")),
        out_specs=(P("rep", None), P("rep", ("fs", "tp")), P(("fs", "tp"), "rep")),
        check_vma=False,
    )
```

```python
import functools

import jax
import jax.numpy as jnp
from jax import lax
from jax.experimental import pallas as pl
from jax.experimental.pallas import tpu as pltpu
from jax.sharding import PartitionSpec as P

MESH = pl.DeviceIdType.MESH
BF16, F32 = jnp.bfloat16, jnp.float32


def contract_last(left, right):
    return lax.dot_general(left, right, (((1,), (1,)), ((), ())), preferred_element_type=F32)


def contract_first(left, right):
    return lax.dot_general(left, right, (((0,), (0,)), ((), ())), preferred_element_type=F32)


def plain(hidden_in, cotangent, w_up, w_down):
    up_full = lax.all_gather(w_up, "rep", axis=0, tiled=True)
    back_grad = contract_last(cotangent, lax.all_gather(w_down, "rep", axis=1, tiled=True))
    preact = jnp.dot(hidden_in, up_full, preferred_element_type=F32)
    active = jnp.maximum(preact, 0.0)
    hidden = (active * active).astype(BF16)
    slopes = (2.0 * active * back_grad).astype(BF16)
    grad_upper = lax.psum_scatter(
        contract_first(hidden_in, slopes).astype(BF16), "rep", scatter_dimension=0, tiled=True
    ).astype(F32)
    lower_rows = lax.psum_scatter(
        contract_first(cotangent, hidden).astype(BF16), "rep", scatter_dimension=0, tiled=True
    ).astype(F32)
    partial_sum = contract_last(slopes, up_full).astype(BF16)
    input_grad = lax.psum(partial_sum, ("fs", "tp")).astype(F32).astype(BF16)
    return (input_grad, grad_upper, lower_rows.T)


SEMS = 256


def kernel(
    R, x_ref, g_ref, wu_in, wd_in,
    ig_ref, ru_ref, rd_ref,
    tx, tg, wu, wd, act, slopes, s_t, h_t, part, r0, r1, r2, r3, ug, dg,
    send_sems, recv_sems, local_sems,
):
    z, f, c = lax.axis_index("rep"), lax.axis_index("fs"), lax.axis_index("tp")
    tl, D = x_ref.shape
    dl, fl = wu_in.shape
    h = fl // R
    pr = tl // 8
    xx, yy = lax.rem(f, 2), lax.div(f, 2)
    fx, fy = yy * 2 + (1 - xx), (1 - yy) * 2 + xx
    f1 = fx * (1 - c) + fy * c
    f2 = fy * (1 - c) + fx * c
    f3 = 3 - f

    edge = jnp.minimum(z, R - 1 - z)
    far = jnp.where(z < R - 1 - z, 1, -1)

    def plane_at(slot):
        both = z + (slot // 2 + 1) * (2 * (slot % 2) - 1) * far
        return jnp.where(slot < 2 * edge, both, z + far * (slot + 1 - edge))

    near_first = [plane_at(slot) for slot in range(R - 1)]
    far_first = near_first[::-1]

    def beyond(p):
        return jnp.logical_or(jnp.logical_and(p < z, z < R - 1), jnp.logical_and(p > z, z > 0))

    def past(p):
        return jnp.where(p < z, z + 1, z - 1)

    def toward(p):
        return jnp.where(p > z, z + 1, z - 1)

    pending = []
    keys = {}

    def key_of(key, p):
        return keys.setdefault(key, len(keys)) * R + p

    def dev(zz=None, ff=None, cc=None):
        return {"rep": z if zz is None else zz, "fs": f if ff is None else ff, "tp": c if cc is None else cc}

    def send(src, dst, device, key, p, when=None):
        copy = pltpu.make_async_remote_copy(
            src_ref=src, dst_ref=dst, send_sem=send_sems.at[len(pending)],
            recv_sem=recv_sems.at[key_of(key, p)], device_id=device, device_id_type=MESH)
        pending.append((copy, when))
        if when is None:
            copy.start()
        else:
            pl.when(when)(copy.start)

    def arrived(dst, key, p):
        pltpu.make_async_remote_copy(
            src_ref=dst, dst_ref=dst, send_sem=send_sems.at[0],
            recv_sem=recv_sems.at[key_of(key, p)], device_id=dev(cc=1 - c), device_id_type=MESH).wait_recv()

    def rows(zz, ff, cc):
        return pl.ds(pl.multiple_of(zz * tl + (cc * 4 + ff) * pr, pr), pr)

    def piece_rows(ff, cc):
        return pl.ds(pl.multiple_of((cc * 4 + ff) * pr, pr), pr)

    barrier = pltpu.get_barrier_semaphore()
    near = [dev(zz=lax.rem(z + d, R)) for d in range(1, R)] + [dev(ff=fx), dev(ff=fy), dev(cc=1 - c)]
    for device in near:
        pl.semaphore_signal(barrier, inc=1, device_id=device, device_id_type=MESH)
    pl.semaphore_wait(barrier, len(near))

    tokens = (tx, tg)
    sources = (x_ref, g_ref)

    def up_cols(zz):
        return pl.ds(pl.multiple_of(zz * h, h), h)

    def d_block(zz):
        return pl.ds(pl.multiple_of(zz * dl, dl), dl)

    for a in (0, 1):
        for to, there in ((z + 1, z < R - 1), (z - 1, z > 0)):
            send(sources[a].at[piece_rows(f, c), :], tokens[a].at[rows(z, f, c), :],
                 dev(zz=to), ("tok", a, 0), z, when=there)

    own_rows = pl.ds(pl.multiple_of(z * tl, tl), tl)
    local = [
        pltpu.make_async_copy(x_ref, tx.at[own_rows, :], local_sems.at[0]),
        pltpu.make_async_copy(g_ref, tg.at[own_rows, :], local_sems.at[1]),
        pltpu.make_async_copy(wu_in.at[:, up_cols(z)], wu.at[d_block(z), :], local_sems.at[2]),
        pltpu.make_async_copy(wd_in.at[up_cols(z), :], wd.at[:, d_block(z)], local_sems.at[3]),
    ]
    for copy in local:
        copy.start()

    def send_weights(planes):
        for p in planes:
            send(wu_in.at[:, up_cols(p)], wu.at[d_block(z), :], dev(zz=p), ("wu",), z)
        for p in planes:
            send(wd_in.at[up_cols(p), :], wd.at[:, d_block(z)], dev(zz=p), ("wd",), z)

    def spread(at, tag, p):
        def first():
            mine = at(f, c)
            send(mine, mine, dev(ff=f1), tag + (1,), p)
            send(mine, mine, dev(ff=f2), tag + (2,), p)
            send(mine, mine, dev(cc=1 - c), tag + (4,), p)

        def second():
            p1, p2 = at(f1, c), at(f2, c)
            arrived(p1, tag + (1,), p)
            send(p1, p1, dev(ff=f2), tag + (3,), p)
            send(p1, p1, dev(cc=1 - c), tag + (5,), p)
            arrived(p2, tag + (2,), p)
            send(p2, p2, dev(cc=1 - c), tag + (6,), p)

        def third():
            p3 = at(f3, c)
            arrived(p3, tag + (3,), p)
            send(p3, p3, dev(cc=1 - c), tag + (7,), p)

        def last():
            for k, ff in ((4, f), (5, f2), (6, f1), (7, f3)):
                arrived(at(ff, 1 - c), tag + (k,), p)

        return first, second, third, last

    lasts = {}
    stages = []
    for a in (0, 1):
        for slot, p in enumerate(near_first):
            first, second, third, last = spread(
                lambda ff, cc, a=a, p=p: tokens[a].at[rows(p, ff, cc), :], ("tok", a), p)

            def opening(a=a, p=p, first=first):
                mine = tokens[a].at[rows(p, f, c), :]
                arrived(mine, ("tok", a, 0), p)
                send(mine, mine, dev(zz=past(p)), ("tok", a, 0), p, when=beyond(p))
                first()

            stages.append((opening, second, third))
            lasts[a, slot] = last
    step = min(tl, 256)

    def up_block(p):
        @pl.loop(0, tl // step)
        def _(i):
            at = pl.ds(pl.multiple_of(p * tl + i * step, step), step)
            active = jnp.maximum(jnp.dot(tx[at, :], wu[...], preferred_element_type=F32), 0.0)
            act[at, :] = active
            h_t[:, at] = jnp.transpose(active * active).astype(BF16)

    def up_blocks():
        for copy in local:
            copy.wait()
        for p in near_first:
            arrived(wu.at[d_block(p), :], ("wu",), p)
        up_block(z)
        for slot, p in enumerate(near_first):
            lasts[0, slot]()
            up_block(p)

    for i in range(len(stages) + 2):
        if i == len(stages) + 1:
            up_blocks()
        for back in (0, 1, 2):
            if 0 <= i - back < len(stages):
                stages[i - back][back]()
        if i == R - 1:
            send_weights(far_first[:R // 2])
        if i == len(stages) - 1:
            send_weights(far_first[R // 2:])

    for slot in range(R - 1):
        lasts[1, slot]()

    def down_part(p):
        at = d_block(p)
        dg[:, at] = jnp.dot(h_t[...], tg[:, at], preferred_element_type=F32).astype(BF16)

    for p in far_first:
        down_part(p)
        send(dg.at[:, d_block(p)], rd_ref.at[up_cols(z), :], dev(zz=p), ("rd",), z)
    down_part(z)
    rd_ref[up_cols(z), :] = dg[:, d_block(z)]

    for p in near_first:
        arrived(wd.at[:, d_block(p)], ("wd",), p)

    half = 4 * pr
    blocks = far_first + [z]

    def r0_rows(j, ff=None):
        if ff is None:
            return pl.ds(j * half, half)
        return pl.ds(pl.multiple_of(j * half + ff * pr, pr), pr)

    def added(*terms):
        total = terms[0].astype(F32)
        for term in terms[1:]:
            total = total + term.astype(F32)
        return total.astype(BF16)

    def core_sum(j):
        p = blocks[j]
        arrived(r0.at[r0_rows(j), :], ("r0", j), 0)
        for k, ff in ((1, f3), (0, f1), (None, f2), (None, f)):
            at = rows(p, ff, c)
            part[at, :] = added(part[at, :], r0[r0_rows(j, ff), :])
            if k is not None:
                send(part.at[at, :], r1.at[j, k], dev(ff=f1), ("r1", j, k), 0)

    for j, p in enumerate(blocks):
        @pl.loop(0, tl // step)
        def _(i, p=p):
            at = pl.ds(pl.multiple_of(p * tl + i * step, step), step)
            value = 2.0 * act[at, :] * contract_last(tg[at, :], wd[...])
            slopes[at, :] = value.astype(BF16)
            s_t[:, at] = jnp.transpose(value).astype(BF16)
            part[at, :] = contract_last(slopes[at, :], wu[...]).astype(BF16)

        theirs = pl.ds(pl.multiple_of(p * tl + (1 - c) * half, half), half)
        send(part.at[theirs, :], r0.at[r0_rows(j), :], dev(cc=1 - c), ("r0", j), 0)
        if j:
            core_sum(j - 1)
    core_sum(R - 1)

    def first_sum(j):
        for k, ff in ((1, f2), (0, f)):
            at = rows(blocks[j], ff, c)
            arrived(r1.at[j, k], ("r1", j, k), 0)
            part[at, :] = added(part[at, :], r1[j, k])
            if k:
                send(part.at[at, :], r2.at[j], dev(ff=f2), ("r2", j), 0)

    def second_sum(j):
        p = blocks[j]
        at = rows(p, f, c)
        arrived(r2.at[j], ("r2", j), 0)
        part[at, :] = added(part[at, :], r2[j])

    def line_sum(j):
        p = blocks[j]
        at = rows(p, f, c)
        side = jnp.where(p > z, 0, 1)

        @pl.when(beyond(p))
        def _():
            arrived(r3.at[p, side], ("r3",), p * 2 + side)
            part[at, :] = added(part[at, :], r3[p, side])

        send(part.at[at, :], r3.at[p, side], dev(zz=toward(p)), ("r3",), p * 2 + side)

    def own_sum():
        at = rows(z, f, c)
        for side, there in ((0, z > 0), (1, z < R - 1)):
            @pl.when(there)
            def _(side=side):
                arrived(r3.at[z, side], ("r3",), z * 2 + side)
                part[at, :] = added(part[at, :], r3[z, side])
        ig_ref[piece_rows(f, c), :] = part[at, :]

    def up_part(p):
        at = d_block(p)
        ug[at, :] = jnp.transpose(jnp.dot(s_t[...], tx[:, at], preferred_element_type=F32)).astype(BF16)

    chain = (first_sum, second_sum, line_sum)
    key_of(("r3",), 0)
    key_of("above", 0)
    for i in range(R + 2):
        for back in (2, 1, 0):
            j = i - back
            if 0 <= j < R and not (back == 2 and j == R - 1):
                chain[back](j)
        if i < R - 1:
            p = far_first[i]
            up_part(p)
            send(ug.at[d_block(p), :], ru_ref.at[:, up_cols(z)], dev(zz=p), ("ru",), z)
        if i == R - 1:
            up_part(z)
            ru_ref[:, up_cols(z)] = ug[d_block(z), :]

    own_sum()
    for stage in spread(lambda ff, cc: ig_ref.at[piece_rows(ff, cc), :], ("ig",), 0):
        stage()

    for p in near_first:
        arrived(rd_ref.at[up_cols(p), :], ("rd",), p)
        arrived(ru_ref.at[:, up_cols(p)], ("ru",), p)
    for copy, when in pending:
        if when is None:
            copy.wait_send()
        else:
            pl.when(when)(copy.wait_send)
    assert len(pending) <= SEMS and len(keys) * R <= SEMS


def in_planes(R, hidden_in, cotangent, w_up, w_down):
    tl, D = hidden_in.shape
    dl, fl = w_up.shape
    T, h, pr = tl * R, fl // R, tl // 8
    vmem = pl.BlockSpec(memory_space=pltpu.VMEM)
    input_grad, up, down = pl.pallas_call(
        functools.partial(kernel, R),
        out_shape=(
            jax.ShapeDtypeStruct((tl, D), BF16),
            jax.ShapeDtypeStruct((dl, fl), BF16),
            jax.ShapeDtypeStruct((fl, dl), BF16),
        ),
        in_specs=[pl.BlockSpec(memory_space=pl.ANY)] * 4,
        out_specs=(vmem, vmem, vmem),
        scratch_shapes=[
            pltpu.VMEM((T, D), BF16),
            pltpu.VMEM((T, D), BF16),
            pltpu.VMEM((D, h), BF16),
            pltpu.VMEM((h, D), BF16),
            pltpu.VMEM((T, h), F32),
            pltpu.VMEM((T, h), BF16),
            pltpu.VMEM((h, T), BF16),
            pltpu.VMEM((h, T), BF16),
            pltpu.VMEM((T, D), BF16),
            pltpu.VMEM((R * 4 * pr, D), BF16),
            pltpu.VMEM((R, 2, pr, D), BF16),
            pltpu.VMEM((R, pr, D), BF16),
            pltpu.VMEM((R, 2, pr, D), BF16),
            pltpu.VMEM((D, h), BF16),
            pltpu.VMEM((h, D), BF16),
            pltpu.SemaphoreType.DMA((SEMS,)),
            pltpu.SemaphoreType.DMA((SEMS,)),
            pltpu.SemaphoreType.DMA((4,)),
        ],
        compiler_params=pltpu.CompilerParams(
            collective_id=0, has_side_effects=True, vmem_limit_bytes=65000 * 1024
        ),
    )(hidden_in, cotangent, w_up, w_down)
    return input_grad, up.astype(F32), down.astype(F32)


def solution(mesh):
    R, F, C = (mesh.shape[name] for name in ("rep", "fs", "tp"))
    body = functools.partial(in_planes, R) if (F, C) == (4, 2) else plain
    return jax.shard_map(
        body,
        mesh=mesh,
        in_specs=(P("rep", None), P("rep", None), P("rep", ("fs", "tp")), P(("fs", "tp"), "rep")),
        out_specs=(P("rep", None), P("rep", ("fs", "tp")), P(("fs", "tp"), "rep")),
        check_vma=False,
    )
```

```python
import functools

import jax
import jax.numpy as jnp
from jax import lax
from jax.experimental import pallas as pl
from jax.experimental.pallas import tpu as pltpu
from jax.sharding import PartitionSpec as P

MESH = pl.DeviceIdType.MESH
BF16, F32 = jnp.bfloat16, jnp.float32


def contract_last(left, right):
    return lax.dot_general(left, right, (((1,), (1,)), ((), ())), preferred_element_type=F32)


def contract_first(left, right):
    return lax.dot_general(left, right, (((0,), (0,)), ((), ())), preferred_element_type=F32)


def plain(hidden_in, cotangent, w_up, w_down):
    up_full = lax.all_gather(w_up, "rep", axis=0, tiled=True)
    back_grad = contract_last(cotangent, lax.all_gather(w_down, "rep", axis=1, tiled=True))
    preact = jnp.dot(hidden_in, up_full, preferred_element_type=F32)
    active = jnp.maximum(preact, 0.0)
    hidden = (active * active).astype(BF16)
    slopes = (2.0 * active * back_grad).astype(BF16)
    grad_upper = lax.psum_scatter(
        contract_first(hidden_in, slopes).astype(BF16), "rep", scatter_dimension=0, tiled=True
    ).astype(F32)
    lower_rows = lax.psum_scatter(
        contract_first(cotangent, hidden).astype(BF16), "rep", scatter_dimension=0, tiled=True
    ).astype(F32)
    partial_sum = contract_last(slopes, up_full).astype(BF16)
    input_grad = lax.psum(partial_sum, ("fs", "tp")).astype(F32).astype(BF16)
    return (input_grad, grad_upper, lower_rows.T)


SEMS = 256


def kernel(
    R, x_ref, g_ref, wu_in, wd_in,
    ig_ref, ru_ref, rd_ref,
    tx, tg, wu, wd, act, slopes, s_t, h_t, part, r0, r1, r2, r3, ug, dg,
    send_sems, recv_sems, local_sems,
):
    z, f, c = lax.axis_index("rep"), lax.axis_index("fs"), lax.axis_index("tp")
    tl, D = x_ref.shape
    dl, fl = wu_in.shape
    h = fl // R
    pr = tl // 8
    xx, yy = lax.rem(f, 2), lax.div(f, 2)
    fx, fy = yy * 2 + (1 - xx), (1 - yy) * 2 + xx
    f1 = fx * (1 - c) + fy * c
    f2 = fy * (1 - c) + fx * c
    f3 = 3 - f

    edge = jnp.minimum(z, R - 1 - z)
    far = jnp.where(z < R - 1 - z, 1, -1)

    def plane_at(slot):
        both = z + (slot // 2 + 1) * (2 * (slot % 2) - 1) * far
        return jnp.where(slot < 2 * edge, both, z + far * (slot + 1 - edge))

    near_first = [plane_at(slot) for slot in range(R - 1)]
    far_first = near_first[::-1]

    def beyond(p):
        return jnp.logical_or(jnp.logical_and(p < z, z < R - 1), jnp.logical_and(p > z, z > 0))

    def past(p):
        return jnp.where(p < z, z + 1, z - 1)

    def toward(p):
        return jnp.where(p > z, z + 1, z - 1)

    pending = []
    keys = {}

    def key_of(key, p):
        return keys.setdefault(key, len(keys)) * R + p

    def dev(zz=None, ff=None, cc=None):
        return {"rep": z if zz is None else zz, "fs": f if ff is None else ff, "tp": c if cc is None else cc}

    def send(src, dst, device, key, p, when=None):
        copy = pltpu.make_async_remote_copy(
            src_ref=src, dst_ref=dst, send_sem=send_sems.at[len(pending)],
            recv_sem=recv_sems.at[key_of(key, p)], device_id=device, device_id_type=MESH)
        pending.append((copy, when))
        if when is None:
            copy.start()
        else:
            pl.when(when)(copy.start)

    def arrived(dst, key, p):
        pltpu.make_async_remote_copy(
            src_ref=dst, dst_ref=dst, send_sem=send_sems.at[0],
            recv_sem=recv_sems.at[key_of(key, p)], device_id=dev(cc=1 - c), device_id_type=MESH).wait_recv()

    def rows(zz, ff, cc):
        return pl.ds(pl.multiple_of(zz * tl + (cc * 4 + ff) * pr, pr), pr)

    def piece_rows(ff, cc):
        return pl.ds(pl.multiple_of((cc * 4 + ff) * pr, pr), pr)

    barrier = pltpu.get_barrier_semaphore()
    near = [dev(zz=lax.rem(z + d, R)) for d in range(1, R)] + [dev(ff=fx), dev(ff=fy), dev(cc=1 - c)]
    for device in near:
        pl.semaphore_signal(barrier, inc=1, device_id=device, device_id_type=MESH)
    pl.semaphore_wait(barrier, len(near))

    tokens = (tx, tg)
    sources = (x_ref, g_ref)

    def up_cols(zz):
        return pl.ds(pl.multiple_of(zz * h, h), h)

    def d_block(zz):
        return pl.ds(pl.multiple_of(zz * dl, dl), dl)

    for a in (0, 1):
        for to, there in ((z + 1, z < R - 1), (z - 1, z > 0)):
            send(sources[a].at[piece_rows(f, c), :], tokens[a].at[rows(z, f, c), :],
                 dev(zz=to), ("tok", a, 0), z, when=there)

    own_rows = pl.ds(pl.multiple_of(z * tl, tl), tl)
    local = [
        pltpu.make_async_copy(x_ref, tx.at[own_rows, :], local_sems.at[0]),
        pltpu.make_async_copy(g_ref, tg.at[own_rows, :], local_sems.at[1]),
        pltpu.make_async_copy(wu_in.at[:, up_cols(z)], wu.at[d_block(z), :], local_sems.at[2]),
        pltpu.make_async_copy(wd_in.at[up_cols(z), :], wd.at[:, d_block(z)], local_sems.at[3]),
    ]
    for copy in local:
        copy.start()

    def send_weights(planes):
        for p in planes:
            send(wu_in.at[:, up_cols(p)], wu.at[d_block(z), :], dev(zz=p), ("wu",), z)
        for p in planes:
            send(wd_in.at[up_cols(p), :], wd.at[:, d_block(z)], dev(zz=p), ("wd",), z)

    def spread(at, tag, p):
        def first():
            mine = at(f, c)
            send(mine, mine, dev(ff=f1), tag + (1,), p)
            send(mine, mine, dev(ff=f2), tag + (2,), p)
            send(mine, mine, dev(cc=1 - c), tag + (4,), p)

        def second():
            p1, p2 = at(f1, c), at(f2, c)
            arrived(p1, tag + (1,), p)
            send(p1, p1, dev(ff=f2), tag + (3,), p)
            send(p1, p1, dev(cc=1 - c), tag + (5,), p)
            arrived(p2, tag + (2,), p)
            send(p2, p2, dev(cc=1 - c), tag + (6,), p)

        def third():
            p3 = at(f3, c)
            arrived(p3, tag + (3,), p)
            send(p3, p3, dev(cc=1 - c), tag + (7,), p)

        def last():
            for k, ff in ((4, f), (5, f2), (6, f1), (7, f3)):
                arrived(at(ff, 1 - c), tag + (k,), p)

        return first, second, third, last

    lasts = {}
    stages = []
    for a in (0, 1):
        for slot, p in enumerate(near_first):
            first, second, third, last = spread(
                lambda ff, cc, a=a, p=p: tokens[a].at[rows(p, ff, cc), :], ("tok", a), p)

            def opening(a=a, p=p, first=first):
                mine = tokens[a].at[rows(p, f, c), :]
                arrived(mine, ("tok", a, 0), p)
                send(mine, mine, dev(zz=past(p)), ("tok", a, 0), p, when=beyond(p))
                first()

            stages.append((opening, second, third))
            lasts[a, slot] = last
    step = min(tl, 256)

    def up_block(p):
        @pl.loop(0, tl // step)
        def _(i):
            at = pl.ds(pl.multiple_of(p * tl + i * step, step), step)
            active = jnp.maximum(jnp.dot(tx[at, :], wu[...], preferred_element_type=F32), 0.0)
            act[at, :] = active
            h_t[:, at] = jnp.transpose(active * active).astype(BF16)

    def up_blocks():
        for copy in local:
            copy.wait()
        for p in near_first:
            arrived(wu.at[d_block(p), :], ("wu",), p)
        up_block(z)
        for slot, p in enumerate(near_first):
            lasts[0, slot]()
            up_block(p)

    for i in range(len(stages) + 2):
        if i == len(stages) + 1:
            up_blocks()
        for back in (0, 1, 2):
            if 0 <= i - back < len(stages):
                stages[i - back][back]()
        if i == R - 1:
            send_weights(far_first[:R // 2])
        if i == len(stages) - 1:
            send_weights(far_first[R // 2:])

    for slot in range(R - 1):
        lasts[1, slot]()

    def down_part(p):
        at = d_block(p)
        dg[:, at] = jnp.dot(h_t[...], tg[:, at], preferred_element_type=F32).astype(BF16)

    for p in far_first:
        down_part(p)
        send(dg.at[:, d_block(p)], rd_ref.at[up_cols(z), :], dev(zz=p), ("rd",), z)
    down_part(z)
    rd_ref[up_cols(z), :] = dg[:, d_block(z)]

    for p in near_first:
        arrived(wd.at[:, d_block(p)], ("wd",), p)

    half = 4 * pr
    blocks = far_first + [z]

    def r0_rows(j, ff=None):
        if ff is None:
            return pl.ds(j * half, half)
        return pl.ds(pl.multiple_of(j * half + ff * pr, pr), pr)

    def added(*terms):
        total = terms[0].astype(F32)
        for term in terms[1:]:
            total = total + term.astype(F32)
        return total.astype(BF16)

    def core_sum(j):
        p = blocks[j]
        arrived(r0.at[r0_rows(j), :], ("r0", j), 0)
        for k, ff in ((1, f3), (0, f1), (None, f2), (None, f)):
            at = rows(p, ff, c)
            part[at, :] = added(part[at, :], r0[r0_rows(j, ff), :])
            if k is not None:
                send(part.at[at, :], r1.at[j, k], dev(ff=f1), ("r1", j, k), 0)

    for j, p in enumerate(blocks):
        @pl.loop(0, tl // step)
        def _(i, p=p):
            at = pl.ds(pl.multiple_of(p * tl + i * step, step), step)
            value = 2.0 * act[at, :] * contract_last(tg[at, :], wd[...])
            slopes[at, :] = value.astype(BF16)
            s_t[:, at] = jnp.transpose(value).astype(BF16)
            part[at, :] = contract_last(slopes[at, :], wu[...]).astype(BF16)

        theirs = pl.ds(pl.multiple_of(p * tl + (1 - c) * half, half), half)
        send(part.at[theirs, :], r0.at[r0_rows(j), :], dev(cc=1 - c), ("r0", j), 0)
        if j:
            core_sum(j - 1)
    core_sum(R - 1)

    def first_sum(j):
        for k, ff in ((1, f2), (0, f)):
            at = rows(blocks[j], ff, c)
            arrived(r1.at[j, k], ("r1", j, k), 0)
            part[at, :] = added(part[at, :], r1[j, k])
            if k:
                send(part.at[at, :], r2.at[j], dev(ff=f2), ("r2", j), 0)

    def second_sum(j):
        p = blocks[j]
        at = rows(p, f, c)
        arrived(r2.at[j], ("r2", j), 0)
        part[at, :] = added(part[at, :], r2[j])

    def line_sum(j):
        p = blocks[j]
        at = rows(p, f, c)
        side = jnp.where(p > z, 0, 1)

        @pl.when(beyond(p))
        def _():
            arrived(r3.at[p, side], ("r3",), p * 2 + side)
            part[at, :] = added(part[at, :], r3[p, side])

        send(part.at[at, :], r3.at[p, side], dev(zz=toward(p)), ("r3",), p * 2 + side)

    def own_sum():
        at = rows(z, f, c)
        for side, there in ((0, z > 0), (1, z < R - 1)):
            @pl.when(there)
            def _(side=side):
                arrived(r3.at[z, side], ("r3",), z * 2 + side)
                part[at, :] = added(part[at, :], r3[z, side])
        ig_ref[piece_rows(f, c), :] = part[at, :]

    def up_part(p):
        at = d_block(p)
        ug[at, :] = jnp.transpose(jnp.dot(s_t[...], tx[:, at], preferred_element_type=F32)).astype(BF16)

    chain = (first_sum, second_sum, line_sum)
    key_of(("r3",), 0)
    key_of("above", 0)
    for i in range(R + 2):
        for back in (2, 1, 0):
            j = i - back
            if 0 <= j < R and not (back == 2 and j == R - 1):
                chain[back](j)
        if i < R - 1:
            p = far_first[i]
            up_part(p)
            send(ug.at[d_block(p), :], ru_ref.at[:, up_cols(z)], dev(zz=p), ("ru",), z)
        if i == R - 1:
            up_part(z)
            ru_ref[:, up_cols(z)] = ug[d_block(z), :]

    own_sum()
    def part_of(n):
        rows_of = lambda ff, cc: pl.ds(pl.multiple_of((cc * 4 + ff) * pr + n * (pr // 2), pr // 2), pr // 2)
        return spread(lambda ff, cc: ig_ref.at[rows_of(ff, cc), :], ("ig", n), 0)

    for pair in zip(part_of(0), part_of(1)):
        for stage in pair:
            stage()

    for p in near_first:
        arrived(rd_ref.at[up_cols(p), :], ("rd",), p)
        arrived(ru_ref.at[:, up_cols(p)], ("ru",), p)
    for copy, when in pending:
        if when is None:
            copy.wait_send()
        else:
            pl.when(when)(copy.wait_send)
    assert len(pending) <= SEMS and len(keys) * R <= SEMS


def in_planes(R, hidden_in, cotangent, w_up, w_down):
    tl, D = hidden_in.shape
    dl, fl = w_up.shape
    T, h, pr = tl * R, fl // R, tl // 8
    vmem = pl.BlockSpec(memory_space=pltpu.VMEM)
    input_grad, up, down = pl.pallas_call(
        functools.partial(kernel, R),
        out_shape=(
            jax.ShapeDtypeStruct((tl, D), BF16),
            jax.ShapeDtypeStruct((dl, fl), BF16),
            jax.ShapeDtypeStruct((fl, dl), BF16),
        ),
        in_specs=[pl.BlockSpec(memory_space=pl.ANY)] * 4,
        out_specs=(vmem, vmem, vmem),
        scratch_shapes=[
            pltpu.VMEM((T, D), BF16),
            pltpu.VMEM((T, D), BF16),
            pltpu.VMEM((D, h), BF16),
            pltpu.VMEM((h, D), BF16),
            pltpu.VMEM((T, h), F32),
            pltpu.VMEM((T, h), BF16),
            pltpu.VMEM((h, T), BF16),
            pltpu.VMEM((h, T), BF16),
            pltpu.VMEM((T, D), BF16),
            pltpu.VMEM((R * 4 * pr, D), BF16),
            pltpu.VMEM((R, 2, pr, D), BF16),
            pltpu.VMEM((R, pr, D), BF16),
            pltpu.VMEM((R, 2, pr, D), BF16),
            pltpu.VMEM((D, h), BF16),
            pltpu.VMEM((h, D), BF16),
            pltpu.SemaphoreType.DMA((SEMS,)),
            pltpu.SemaphoreType.DMA((SEMS,)),
            pltpu.SemaphoreType.DMA((4,)),
        ],
        compiler_params=pltpu.CompilerParams(
            collective_id=0, has_side_effects=True, vmem_limit_bytes=65000 * 1024
        ),
    )(hidden_in, cotangent, w_up, w_down)
    return input_grad, up.astype(F32), down.astype(F32)


def solution(mesh):
    R, F, C = (mesh.shape[name] for name in ("rep", "fs", "tp"))
    body = functools.partial(in_planes, R) if (F, C) == (4, 2) else plain
    return jax.shard_map(
        body,
        mesh=mesh,
        in_specs=(P("rep", None), P("rep", None), P("rep", ("fs", "tp")), P(("fs", "tp"), "rep")),
        out_specs=(P("rep", None), P("rep", ("fs", "tp")), P(("fs", "tp"), "rep")),
        check_vma=False,
    )
```
